32 devices in a mesh: rep: 2 (over x), fs: 8 (over z, y), tp: 2 (over core).
Axes of the slice: x: 2, y: 2, z: 4, core: 2. Of those that a mesh axis runs over, the one named last changes fastest.
Arguments:
- tokens: bfloat16 [5120, 2048], P(('rep', 'fs'), 'tp'), may hold values from -30 to 30
- mixer_gain: float32 [2048], P('tp'), may hold values from 0.1 to 1.9
- outer_weight: float32 [2048, 1024], P('fs', 'tp'), may hold values from -0.125 to 0.125
- inner_weight: float32 [2048, 1024], P('fs', 'tp'), may hold values from -0.125 to 0.125
- value_weight: float32 [2048, 1024], P('fs', 'tp'), may hold values from -0.125 to 0.125
- outer_scale: float32 [1024], P(('tp', 'fs')), may hold values from 0.5 to 2
- inner_scale: float32 [1024], P(('tp', 'fs')), may hold values from 0.5 to 2
- value_scale: float32 [1024], P(('tp', 'fs')), may hold values from 0.5 to 2
- mixer_taps: float32 [3, 1024], P(None, 'tp'), may hold values from -3.5 to 3.5
- mixer_project: float32 [1024, 2048], P('tp', 'fs'), may hold values from -0.1875 to 0.1875
- project_scale: float32 [2048], P('fs'), may hold values from 0.5 to 2
- channel_gain: float32 [2048], P('tp'), may hold values from 0.1 to 1.9
- gate_weight: float32 [2048, 5632], P('fs', 'tp'), may hold values from -0.125 to 0.125
- gate_scale: float32 [5632], P(('tp', 'fs')), may hold values from 0.5 to 2
- up_weight: float32 [2048, 5632], P('fs', 'tp'), may hold values from -0.125 to 0.125
- up_scale: float32 [5632], P(('tp', 'fs')), may hold values from 0.5 to 2
- channel_taps: float32 [3, 5632], P(None, 'tp'), may hold values from -3.5 to 3.5
- channel_bias: float32 [5632], P('tp'), may hold values from -3 to 3
- down_weight: float32 [5632, 2048], P('tp', 'fs'), may hold values from -0.078125 to 0.078125
- down_scale: float32 [2048], P('fs'), may hold values from 0.5 to 2
Outputs:
- result: bfloat16 [5120, 2048], P(('rep', 'fs'), 'tp')
The draws below stay inside these ranges and needn't reach their ends.
All inputs are finite; a program needn't handle non-finite values.
Results may differ from the reference program's by a relative error of at most 0.015.
Values may be sent and summed in bfloat16 or wider, within the bound.
A program may use at most 128 MiB of HBM per device.

```python
import math
import jax
import jax.numpy as jnp
from jax import lax

D = 2048
CW = 1024
FF = 5632
TAPS = 3
LEN = 320
TOKENS = 5120
N_TP = 2


def draw_tokens(key, part):
    first_key, second_key, third_key = jax.random.split(jax.random.fold_in(key, 11), 3)
    rough = jnp.exp(jax.random.uniform(second_key, (D,), jnp.float32, -0.7, 0.7))
    row_scale = jnp.exp(jax.random.uniform(third_key, (TOKENS, 1), jnp.float32, math.log(0.3), math.log(3.0)))
    rising = jnp.exp(jnp.linspace(0.0, math.log(3.0), D)).astype(jnp.float32)
    values = jax.random.normal(first_key, (TOKENS, D), jnp.float32) * row_scale * rough * rising
    return jnp.clip(values, -30.0, 30.0).astype(jnp.bfloat16)


def block_levels(stream_key, extent, cuts, smallest, top_value):
    level, own = 1.0, jax.random.fold_in(stream_key, 6)
    for axis_at, blocks in cuts:
        draws = jnp.exp(jax.random.uniform(jax.random.fold_in(own, axis_at), (blocks,), jnp.float32, smallest / len(cuts), top_value / len(cuts)))
        level = level * jnp.repeat(draws, extent[axis_at] // blocks).reshape([-1 if axis == axis_at else 1 for axis in range(len(extent))])
    return level


def centred(stream_key, extent, spread, most, cuts=(), held_as=jnp.bfloat16):
    result = spread * jax.random.normal(stream_key, extent, jnp.float32)
    if cuts:
        result = result * block_levels(stream_key, extent, cuts, -0.22, 0.18)
    return jnp.clip(result, -most, most).astype(held_as)


def setup_inputs(seed: int = 0) -> dict:
    arg_keys = jax.random.split(jax.random.key(seed), 21)
    return {
        "tokens": draw_tokens(jax.random.fold_in(arg_keys[20], 71), 0),
        "mixer_gain": jnp.clip(1.0 + 0.18 * jax.random.normal(arg_keys[1], (D,), jnp.float32), 0.1, 1.9),
        "outer_weight": centred(arg_keys[2], (D, CW), D ** -0.5, 0.125, ((0, 8), (1, 2)), jnp.float32),
        "inner_weight": centred(arg_keys[3], (D, CW), D ** -0.5, 0.125, ((0, 8), (1, 2)), jnp.float32),
        "value_weight": centred(arg_keys[4], (D, CW), D ** -0.5, 0.125, ((0, 8), (1, 2)), jnp.float32),
        "outer_scale": jnp.clip(jnp.exp(math.log(2.0) - 1.3862944 * jax.random.uniform(arg_keys[5], (CW,), jnp.float32) ** block_levels(arg_keys[5], (CW,), ((0, 16),), -0.2, 0.2)), 0.5, 2.0),
        "inner_scale": jnp.clip(jnp.exp(math.log(2.0) - 1.3862944 * jax.random.uniform(arg_keys[6], (CW,), jnp.float32) ** block_levels(arg_keys[6], (CW,), ((0, 16),), -0.2, 0.2)), 0.5, 2.0),
        "value_scale": jnp.clip(jnp.exp(math.log(2.0) - 1.3862944 * jax.random.uniform(arg_keys[7], (CW,), jnp.float32) ** block_levels(arg_keys[7], (CW,), ((0, 16),), -0.2, 0.2)), 0.5, 2.0),
        "mixer_taps": centred(arg_keys[8], (TAPS, CW), TAPS ** -0.5, 3.5, ((1, 2),), jnp.float32),
        "mixer_project": centred(arg_keys[9], (CW, D), CW ** -0.5, 0.1875, ((0, 2), (1, 8)), jnp.float32),
        "project_scale": jnp.clip(jnp.exp(math.log(2.0) - 1.3862944 * jax.random.uniform(arg_keys[10], (D,), jnp.float32) ** block_levels(arg_keys[10], (D,), ((0, 8),), -0.2, 0.2)), 0.5, 2.0),
        "channel_gain": jnp.clip(1.0 + 0.18 * jax.random.normal(arg_keys[11], (D,), jnp.float32), 0.1, 1.9),
        "gate_weight": centred(arg_keys[12], (D, FF), D ** -0.5, 0.125, ((0, 8), (1, 2)), jnp.float32),
        "gate_scale": jnp.clip(jnp.exp(math.log(2.0) - 1.3862944 * jax.random.uniform(arg_keys[13], (FF,), jnp.float32) ** block_levels(arg_keys[13], (FF,), ((0, 16),), -0.2, 0.2)), 0.5, 2.0),
        "up_weight": centred(arg_keys[14], (D, FF), D ** -0.5, 0.125, ((0, 8), (1, 2)), jnp.float32),
        "up_scale": jnp.clip(jnp.exp(math.log(2.0) - 1.3862944 * jax.random.uniform(arg_keys[15], (FF,), jnp.float32) ** block_levels(arg_keys[15], (FF,), ((0, 16),), -0.2, 0.2)), 0.5, 2.0),
        "channel_taps": centred(arg_keys[16], (TAPS, FF), TAPS ** -0.5, 3.5, ((1, 2),), jnp.float32),
        "channel_bias": centred(arg_keys[17], (FF,), 0.5, 3.0, ((0, 2),), jnp.float32),
        "down_weight": centred(arg_keys[18], (FF, D), FF ** -0.5, 0.078125, ((0, 2), (1, 8)), jnp.float32),
        "down_scale": jnp.clip(jnp.exp(math.log(2.0) - 1.3862944 * jax.random.uniform(arg_keys[19], (D,), jnp.float32) ** block_levels(arg_keys[19], (D,), ((0, 8),), -0.2, 0.2)), 0.5, 2.0),
    }


epsilon = 1e-06

def normalize(token_rows, gain):
    values = token_rows.astype(jnp.float32)
    inverse = lax.rsqrt(lax.optimization_barrier(jnp.sum(values * values, axis=1, keepdims=True)) / values.shape[1] + epsilon)
    return (values * inverse * gain.astype(jnp.float32)).astype(jnp.bfloat16)

def causal_taps(values, taps):
    tap_count = taps.shape[0]
    length = values.shape[0]
    padded = jnp.pad(values, ((tap_count - 1, 0), (0, 0)))
    running = jnp.zeros_like(values)
    for offset in range(tap_count):
        running = running + taps[offset].astype(jnp.float32) * padded[offset:offset + length]
    return running

def block_sums(hidden, weight, scale, blocks):
    length, channels = hidden.shape
    pieces = hidden.reshape(length, blocks, channels // blocks).astype(jnp.float32)
    matrices = weight.reshape(blocks, channels // blocks, weight.shape[1]).astype(jnp.float32)
    partials = jnp.einsum('lbc,bcd->bld', pieces, matrices) * scale.astype(jnp.float32)
    rounded = lax.optimization_barrier(partials.astype(jnp.bfloat16))
    return lax.optimization_barrier(jnp.sum(rounded.astype(jnp.float32), axis=0))

def scaled_product(normed, weight, scale):
    return jnp.dot(normed, weight, preferred_element_type=jnp.float32) * scale.astype(jnp.float32)

def reference(tokens, mixer_gain, outer_weight, inner_weight, value_weight, outer_scale, inner_scale, value_scale, mixer_taps, mixer_project, project_scale, channel_gain, gate_weight, gate_scale, up_weight, up_scale, channel_taps, channel_bias, down_weight, down_scale):
    outer_low = outer_weight.astype(jnp.bfloat16)
    inner_low = inner_weight.astype(jnp.bfloat16)
    value_low = value_weight.astype(jnp.bfloat16)
    project_low = mixer_project.astype(jnp.bfloat16)
    gate_low = gate_weight.astype(jnp.bfloat16)
    up_low = up_weight.astype(jnp.bfloat16)
    down_low = down_weight.astype(jnp.bfloat16)

    def one_sequence(token_rows):
        normed = normalize(token_rows, mixer_gain)
        outer_part = scaled_product(normed, outer_low, outer_scale)
        inner_part = scaled_product(normed, inner_low, inner_scale)
        value_part = scaled_product(normed, value_low, value_scale)
        mixed = (outer_part * causal_taps(inner_part * value_part, mixer_taps)).astype(jnp.bfloat16)
        middle = (token_rows.astype(jnp.float32) + block_sums(mixed, project_low, project_scale, N_TP)).astype(jnp.bfloat16)
        normed_two = normalize(middle, channel_gain)
        gate_part = scaled_product(normed_two, gate_low, gate_scale)
        up_part = scaled_product(normed_two, up_low, up_scale)
        hidden = (jax.nn.silu(causal_taps(gate_part, channel_taps) + channel_bias.astype(jnp.float32)) * up_part).astype(jnp.bfloat16)
        return (middle.astype(jnp.float32) + block_sums(hidden, down_low, down_scale, N_TP)).astype(jnp.bfloat16)
    sequences = tokens.reshape(tokens.shape[0] // LEN, LEN, tokens.shape[1])
    return lax.map(one_sequence, sequences).reshape(tokens.shape)
```

```python
import jax
import jax.numpy as jnp
from jax import lax
from jax.sharding import PartitionSpec as P

LEN = 320
GROUPS = 4

epsilon = 1e-06
low = jnp.bfloat16


class Place:
    def __init__(self):
        self.fs = lax.axis_size("fs")
        self.reps = lax.axis_size("rep")
        self.tps = lax.axis_size("tp")
        self.slow = GROUPS if self.fs % GROUPS == 0 else 1
        self.fast = self.fs // self.slow
        at = lax.axis_index("fs")
        self.z, self.y = at // self.fast, at % self.fast
        self.r, self.t = lax.axis_index("rep"), lax.axis_index("tp")

    def from_slow(self, block, shift):
        perm = [(z * self.fast + y, (z - shift) % self.slow * self.fast + y)
                for z in range(self.slow) for y in range(self.fast)]
        return lax.ppermute(block, "fs", perm)

    def from_fast(self, block, shift):
        perm = [(z * self.fast + y, z * self.fast + (y - shift) % self.fast)
                for z in range(self.slow) for y in range(self.fast)]
        return lax.ppermute(block, "fs", perm)

    def from_rep(self, block, shift):
        return lax.ppermute(block, "rep", [(i, (i - shift) % self.reps) for i in range(self.reps)])

    def from_tp(self, block, shift):
        return lax.ppermute(block, "tp", [(i, (i - shift) % self.tps) for i in range(self.tps)])

    def spread(self, pieces, axis):
        held = jnp.concatenate(pieces, axis)
        held = jnp.concatenate([held] + [self.from_fast(held, j) for j in range(1, self.fast)], axis)
        return jnp.concatenate([held] + [self.from_rep(held, i) for i in range(1, self.reps)], axis)

    def order(self, width):
        return [
            (((self.z + k) % self.slow * self.fast + (self.y + j) % self.fast) * self.reps
             + (self.r + i) % self.reps) * width
            for i in range(self.reps) for j in range(self.fast) for k in range(self.slow)
        ]

    def position(self, block):
        f, part = block // self.reps, block % self.reps
        i = (part - self.r) % self.reps
        j = (f % self.fast - self.y) % self.fast
        k = (f // self.fast - self.z) % self.slow
        return (i * self.fast + j) * self.slow + k


def columns(values, offsets, width):
    return jnp.concatenate(
        [lax.dynamic_slice(values, (0, offset), (values.shape[0], width)) for offset in offsets], axis=1
    )


def inverse_norm(place, values):
    own = jnp.sum(values * values, axis=1)
    total = own
    for s in range(1, place.tps):
        total = total + place.from_tp(own, s)
    return lax.rsqrt(total / (values.shape[1] * place.tps) + epsilon)


def normalize(place, token_rows, gain):
    values = token_rows.astype(jnp.float32)
    return (values * inverse_norm(place, values)[:, None] * gain).astype(low)


def all_features(place, local, width):
    held = jnp.concatenate([local] + [place.from_tp(local, s) for s in range(1, place.tps)], axis=1)
    whole = held.shape[1]
    offsets = [(offset - place.t * local.shape[1]) % whole for offset in place.order(width)]
    return columns(held, offsets, width)


def own_features(place, product, width):
    local = product.shape[1] // place.tps
    count = local // width

    def share(peer):
        return columns(product, [place.position(peer * count + b) * width for b in range(count)], width)

    total = share(place.t)
    for s in range(1, place.tps):
        total = total + place.from_tp(share((place.t - s) % place.tps).astype(low), s).astype(jnp.float32)
    return total


def causal_taps(values, taps):
    tap_count = taps.shape[0]
    grouped = values.reshape(-1, LEN, values.shape[1])
    padded = jnp.pad(grouped, ((0, 0), (tap_count - 1, 0), (0, 0)))
    running = jnp.zeros_like(grouped)
    for offset in range(tap_count):
        running = running + taps[offset] * padded[:, offset : offset + LEN]
    return running.reshape(values.shape)


def dot(left, right):
    return jnp.dot(left, right, preferred_element_type=jnp.float32)


def per_device(
    tokens, mixer_gain, outer_weight, inner_weight, value_weight, outer_scale, inner_scale,
    value_scale, mixer_taps, mixer_project, project_scale, channel_gain, gate_weight, gate_scale,
    up_weight, up_scale, channel_taps, channel_bias, down_weight, down_scale,
):
    place = Place()
    rows = outer_weight.shape[0] // place.reps
    width = mixer_project.shape[1] // place.reps
    slow = place.slow
    quarter = gate_weight.shape[1] // slow

    def row_share(weight):
        return lax.dynamic_slice_in_dim(weight, place.r * rows, rows, 0).astype(low)

    def column_share(weight):
        return lax.dynamic_slice_in_dim(weight, place.r * width, width, 1).astype(low)

    def same(piece):
        return [piece] + [place.from_slow(piece, k) for k in range(1, slow)]

    def exchange(take):
        return [take(place.z)] + [
            place.from_slow(take((place.z - k) % slow), k) for k in range(1, slow)
        ]

    mixer_in = place.spread(
        same(jnp.concatenate([row_share(w) for w in (outer_weight, inner_weight, value_weight)], axis=1)), 0
    )
    project = place.spread(same(column_share(mixer_project)), 1)

    def column_part(weight):
        parts = row_share(weight).reshape(rows, slow, quarter).transpose(1, 0, 2)
        return lambda z: lax.dynamic_index_in_dim(parts, z, 0, keepdims=False)

    gate_full = place.spread(exchange(column_part(gate_weight)), 0)
    up_full = place.spread(exchange(column_part(up_weight)), 0)
    down_share = column_share(down_weight)
    down_full = place.spread(
        exchange(lambda z: lax.dynamic_slice_in_dim(down_share, z * quarter, quarter, 0)), 1
    )

    scales = (outer_scale, inner_scale, value_scale, gate_scale, up_scale, project_scale, down_scale)
    packed = lax.all_gather(jnp.concatenate(scales), "fs", axis=0)
    ends, full = 0, []
    for scale in scales:
        full.append(packed[:, ends : ends + scale.shape[0]].reshape(-1))
        ends += scale.shape[0]
    outer_all, inner_all, value_all, gate_all, up_all, project_all, down_all = full
    local = tokens.shape[1]

    def mine(vector, at, size):
        return lax.dynamic_slice_in_dim(vector, at * size, size, vector.ndim - 1)

    normed = all_features(place, normalize(place, tokens, mixer_gain), rows)
    parts = dot(normed, mixer_in)
    each = outer_weight.shape[1]
    outer_part = parts[:, :each] * outer_all
    conv_input = parts[:, each : 2 * each] * inner_all * (parts[:, 2 * each :] * value_all)
    mixed = (outer_part * causal_taps(conv_input, mixer_taps)).astype(low)
    mixer_sum = own_features(place, dot(mixed, project), width) * mine(project_all, place.t, local)
    middle = (tokens.astype(jnp.float32) + mixer_sum).astype(low)

    normed_own = normalize(place, middle, channel_gain)
    normed_two = jnp.concatenate(
        [normed_own] + [place.from_slow(normed_own, k) for k in range(1, slow)], axis=0
    )
    normed_two = all_features(place, normed_two, rows)
    gate_part = dot(normed_two, gate_full) * mine(gate_all, place.z, quarter)
    up_part = dot(normed_two, up_full) * mine(up_all, place.z, quarter)
    hidden = (
        jax.nn.silu(
            causal_taps(gate_part, mine(channel_taps, place.z, quarter))
            + mine(channel_bias, place.z, quarter)
        )
        * up_part
    ).astype(low)
    share = own_features(place, dot(hidden, down_full), width)
    count = tokens.shape[0]
    total = share[:count]
    for k in range(1, slow):
        sent = share[k * count : (k + 1) * count].astype(low)
        total = total + place.from_slow(sent, -k).astype(jnp.float32)
    return (middle.astype(jnp.float32) + total * mine(down_all, place.t, local)).astype(low)


def solution(mesh):
    placed = (
        P(("rep", "fs"), "tp"),
        P("tp"),
        P("fs", "tp"),
        P("fs", "tp"),
        P("fs", "tp"),
        P(("tp", "fs")),
        P(("tp", "fs")),
        P(("tp", "fs")),
        P(None, "tp"),
        P("tp", "fs"),
        P("fs"),
        P("tp"),
        P("fs", "tp"),
        P(("tp", "fs")),
        P("fs", "tp"),
        P(("tp", "fs")),
        P(None, "tp"),
        P("tp"),
        P("tp", "fs"),
        P("fs"),
    )
    return jax.shard_map(
        per_device, mesh=mesh, in_specs=placed, out_specs=P(("rep", "fs"), "tp"), check_vma=False
    )
```

```python
import jax
import jax.numpy as jnp
from jax import lax
from jax.sharding import PartitionSpec as P

LEN = 320
GROUPS = 4

epsilon = 1e-06
low = jnp.bfloat16


class Place:
    def __init__(self):
        self.fs = lax.axis_size("fs")
        self.reps = lax.axis_size("rep")
        self.tps = lax.axis_size("tp")
        self.slow = GROUPS if self.fs % GROUPS == 0 else 1
        self.fast = self.fs // self.slow
        at = lax.axis_index("fs")
        self.z, self.y = at // self.fast, at % self.fast
        self.r, self.t = lax.axis_index("rep"), lax.axis_index("tp")

    def from_slow(self, block, shift):
        perm = [(z * self.fast + y, (z - shift) % self.slow * self.fast + y)
                for z in range(self.slow) for y in range(self.fast)]
        return lax.ppermute(block, "fs", perm)

    def from_fast(self, block, shift):
        perm = [(z * self.fast + y, z * self.fast + (y - shift) % self.fast)
                for z in range(self.slow) for y in range(self.fast)]
        return lax.ppermute(block, "fs", perm)

    def from_rep(self, block, shift):
        return lax.ppermute(block, "rep", [(i, (i - shift) % self.reps) for i in range(self.reps)])

    def from_tp(self, block, shift):
        return lax.ppermute(block, "tp", [(i, (i - shift) % self.tps) for i in range(self.tps)])

    def spread(self, pieces, rep_first):
        shape = pieces[0].shape
        tail = (0,) * len(shape)

        def gather(held, at, count, axis, fetch):
            whole = jnp.zeros(held.shape[:axis] + (count,) + held.shape[axis + 1 :], held.dtype)
            for k in range(count):
                block = fetch(held, k) if k else held
                start = [0] * whole.ndim
                start[axis] = (at + k) % count
                whole = lax.dynamic_update_slice(whole, block, start)
            return whole

        held = jnp.zeros((self.slow, 1, 1) + shape, pieces[0].dtype)
        for k, piece in enumerate(pieces):
            held = lax.dynamic_update_slice(
                held, piece.reshape((1, 1, 1) + shape), ((self.z + k) % self.slow, 0, 0) + tail
            )
        steps = [(self.y, self.fast, 1, self.from_fast), (self.r, self.reps, 2, self.from_rep)]
        if rep_first:
            steps.reverse()
        for at, count, axis, fetch in steps:
            held = gather(held, at, count, axis, fetch)
        return held


def inverse_norm(place, values):
    own = jnp.sum(values * values, axis=1)
    total = own
    for s in range(1, place.tps):
        total = total + place.from_tp(own, s)
    return lax.rsqrt(total / (values.shape[1] * place.tps) + epsilon)


def normalize(place, token_rows, gain):
    values = token_rows.astype(jnp.float32)
    return (values * inverse_norm(place, values)[:, None] * gain).astype(low)


def all_features(place, local):
    size = local.shape[1]
    whole = jnp.zeros((local.shape[0], size * place.tps), local.dtype)
    for k in range(place.tps):
        block = place.from_tp(local, k) if k else local
        whole = lax.dynamic_update_slice(whole, block, (0, (place.t + k) % place.tps * size))
    return whole


def own_features(place, product):
    local = product.shape[1] // place.tps

    def share(peer):
        return lax.dynamic_slice_in_dim(product, peer * local, local, 1)

    total = share(place.t)
    for s in range(1, place.tps):
        total = total + place.from_tp(share((place.t - s) % place.tps).astype(low), s).astype(jnp.float32)
    return total


def causal_taps(values, taps):
    tap_count = taps.shape[0]
    grouped = values.reshape(-1, LEN, values.shape[1])
    padded = jnp.pad(grouped, ((0, 0), (tap_count - 1, 0), (0, 0)))
    running = jnp.zeros_like(grouped)
    for offset in range(tap_count):
        running = running + taps[offset] * padded[:, offset : offset + LEN]
    return running.reshape(values.shape)


def dot(left, right):
    return jnp.dot(left, right, preferred_element_type=jnp.float32)


def per_device(
    tokens, mixer_gain, outer_weight, inner_weight, value_weight, outer_scale, inner_scale,
    value_scale, mixer_taps, mixer_project, project_scale, channel_gain, gate_weight, gate_scale,
    up_weight, up_scale, channel_taps, channel_bias, down_weight, down_scale,
):
    place = Place()
    rows = outer_weight.shape[0] // place.reps
    width = mixer_project.shape[1] // place.reps
    slow = place.slow
    quarter = gate_weight.shape[1] // slow

    def row_share(weight):
        return lax.dynamic_slice_in_dim(weight, place.r * rows, rows, 0).astype(low)

    def column_share(weight):
        return lax.dynamic_slice_in_dim(weight, place.r * width, width, 1).astype(low)

    def same(piece):
        return [piece] + [place.from_slow(piece, k) for k in range(1, slow)]

    def exchange(take):
        return [take(place.z)] + [
            place.from_slow(take((place.z - k) % slow), k) for k in range(1, slow)
        ]

    def as_rows(whole):
        return whole.reshape(-1, whole.shape[-1])

    def as_columns(whole):
        return jnp.moveaxis(whole, 3, 0).reshape(whole.shape[3], -1)

    scales = (outer_scale, inner_scale, value_scale, gate_scale, up_scale, project_scale, down_scale)
    own = jnp.concatenate(scales).reshape(1, 1, -1)
    packed = jnp.zeros((slow, 1, own.shape[2]), own.dtype)
    for k in range(slow):
        block = place.from_slow(own, k) if k else own
        packed = lax.dynamic_update_slice(packed, block, ((place.z + k) % slow, 0, 0))
    held, packed = packed, jnp.zeros((slow, place.fast, own.shape[2]), own.dtype)
    for j in range(place.fast):
        block = place.from_fast(held, j) if j else held
        packed = lax.dynamic_update_slice(packed, block, (0, (place.y + j) % place.fast, 0))
    packed = packed.reshape(place.fs, -1)

    outer_full = as_rows(place.spread(same(row_share(outer_weight)), True))
    both_full = as_rows(
        place.spread(same(jnp.concatenate([row_share(inner_weight), row_share(value_weight)], 1)), False)
    )
    project = as_columns(place.spread(same(column_share(mixer_project)), True))

    def column_part(weight):
        parts = row_share(weight).reshape(rows, slow, quarter).transpose(1, 0, 2)
        return lambda z: lax.dynamic_index_in_dim(parts, z, 0, keepdims=False)

    gate_full = as_rows(place.spread(exchange(column_part(gate_weight)), True))
    up_full = as_rows(place.spread(exchange(column_part(up_weight)), False))
    down_share = column_share(down_weight)
    down_full = as_columns(
        place.spread(exchange(lambda z: lax.dynamic_slice_in_dim(down_share, z * quarter, quarter, 0)), True)
    )

    ends, full = 0, []
    for scale in scales:
        full.append(packed[:, ends : ends + scale.shape[0]].reshape(-1))
        ends += scale.shape[0]
    outer_all, inner_all, value_all, gate_all, up_all, project_all, down_all = full
    local = tokens.shape[1]

    def mine(vector, at, size):
        return lax.dynamic_slice_in_dim(vector, at * size, size, vector.ndim - 1)

    normed = all_features(place, normalize(place, tokens, mixer_gain))
    each = inner_weight.shape[1]
    outer_part = dot(normed, outer_full) * outer_all
    parts = dot(normed, both_full)
    conv_input = parts[:, :each] * inner_all * (parts[:, each:] * value_all)
    mixed = (outer_part * causal_taps(conv_input, mixer_taps)).astype(low)
    mixer_sum = own_features(place, dot(mixed, project))
    middle = (tokens.astype(jnp.float32) + mixer_sum * mine(project_all, place.t, local)).astype(low)

    normed_own = normalize(place, middle, channel_gain)
    normed_two = jnp.concatenate(
        [normed_own] + [place.from_slow(normed_own, k) for k in range(1, slow)], axis=0
    )
    normed_two = all_features(place, normed_two)
    gate_part = dot(normed_two, gate_full) * mine(gate_all, place.z, quarter)
    up_part = dot(normed_two, up_full) * mine(up_all, place.z, quarter)
    hidden = (
        jax.nn.silu(
            causal_taps(gate_part, mine(channel_taps, place.z, quarter))
            + mine(channel_bias, place.z, quarter)
        )
        * up_part
    ).astype(low)
    share = own_features(place, dot(hidden, down_full))
    count = tokens.shape[0]
    total = share[:count]
    for k in range(1, slow):
        sent = share[k * count : (k + 1) * count].astype(low)
        total = total + place.from_slow(sent, -k).astype(jnp.float32)
    return (middle.astype(jnp.float32) + total * mine(down_all, place.t, local)).astype(low)


def solution(mesh):
    placed = (
        P(("rep", "fs"), "tp"),
        P("tp"),
        P("fs", "tp"),
        P("fs", "tp"),
        P("fs", "tp"),
        P(("tp", "fs")),
        P(("tp", "fs")),
        P(("tp", "fs")),
        P(None, "tp"),
        P("tp", "fs"),
        P("fs"),
        P("tp"),
        P("fs", "tp"),
        P(("tp", "fs")),
        P("fs", "tp"),
        P(("tp", "fs")),
        P(None, "tp"),
        P("tp"),
        P("tp", "fs"),
        P("fs"),
    )


    return jax.shard_map(per_device, mesh=mesh, in_specs=placed, out_specs=P(("rep", "fs"), "tp"), check_vma=False)
```
